32 devices in a mesh: grp: 2 (over y), sp: 8 (over z, core), tp: 2 (over x).
Axes of the slice: x: 2, y: 2, z: 4, core: 2. Of those that a mesh axis runs over, the one named last changes fastest.
Arguments:
- layer_input: bfloat16 [3072, 2048], P(('grp', 'sp', 'tp')), parts along dimension 0, may hold values from -6 to 6
- latent: bfloat16 [3072, 512], P(('grp', 'sp')), parts along dimension 0, may hold values from -6 to 6
- rope_key: bfloat16 [3072, 64], P(('grp', 'sp')), parts along dimension 0, may hold values from -4 to 4
- query_wide: bfloat16 [3072, 1536], P(('grp', 'sp'), 'tp'), parts along dimension 0, may hold values from -18 to 18
- query_narrow: bfloat16 [3072, 1024], P(('grp', 'sp'), 'tp'), parts along dimension 0, may hold values from -18 to 18
- key_up_wide: bfloat16 [512, 1024], P(None, 'tp'), may hold values from -0.25 to 0.25
- value_up_wide: bfloat16 [512, 1024], P(None, 'tp'), may hold values from -0.25 to 0.25
- key_up_narrow: bfloat16 [512, 512], P(None, 'tp'), may hold values from -0.25 to 0.25
- value_up_narrow: bfloat16 [512, 512], P(None, 'tp'), may hold values from -0.25 to 0.25
- out_wide: bfloat16 [1024, 2048], P('tp'), may hold values from -1.1953125 to 1.1953125
- out_narrow: bfloat16 [512, 2048], P('tp'), may hold values from -1.1953125 to 1.1953125
- norm_gain: float32 [2048], replicated, may hold values from 0.1 to 1.9
- gate_weight: bfloat16 [2048, 5632], P('sp', 'tp'), may hold values from -0.125 to 0.125
- value_weight: bfloat16 [2048, 5632], P('sp', 'tp'), may hold values from -0.125 to 0.125
- conv_weight: float32 [3, 5632], P(None, 'tp'), may hold values from -2.5 to 2.5
- down_weight: bfloat16 [5632, 2048], P('tp', 'sp'), may hold values from -0.078125 to 0.078125
Outputs:
- layer_output: bfloat16 [3072, 2048], P(('grp', 'sp', 'tp')), parts along dimension 0
The draws below stay inside these ranges and needn't reach their ends.
There are 2 independent parts, one for each index of `grp`. The reference program is written for one: setup_inputs(seed, part) draws one part's arguments, and reference() takes and returns one part's arrays. A program takes and returns all parts, laid end to end along the dimension named above; an argument that names none is the same for every part. Nothing has to cross between parts.
All inputs are finite; a program needn't handle non-finite values.
Results may differ from the reference program's by a relative error of at most 0.015.
Values may be sent and summed in bfloat16 or wider, within the bound.
A program may use at most 128 MiB of HBM per device.

```python
import math
import jax
import jax.numpy as jnp
from jax import lax

D = 2048
LATENT = 512
ROT = 64
NOPE_W = 128
VAL_W = 128
NOPE_N = 64
VAL_N = 64
HEADS_W = 8
HEADS_N = 8
FF = 5632
CONV = 3
TOK_DEV = 192
TOKENS = 1536
N_TP = 2


def planted_rows(key):
    positions = jnp.arange(TOKENS, dtype=jnp.int32)
    planted = jax.random.randint(jax.random.fold_in(key, 101), (TOKENS,), 0, 48) == 0
    offsets = jax.random.randint(jax.random.fold_in(key, 103), (TOKENS,), TOK_DEV, TOKENS - TOK_DEV + 1)
    target = (positions + offsets) % TOKENS
    rotary = jnp.clip(jax.random.normal(jax.random.fold_in(key, 102), (TOKENS, ROT), jnp.float32), -4.0, 4.0)
    return (planted, target, rotary)


def planted_query(key, head_count, nope_width, salt_value):
    planted, target, rotary = planted_rows(key)
    own_key = jax.random.fold_in(key, salt_value)
    drawn = jnp.clip(2.0 * jax.random.normal(own_key, (TOKENS, head_count, nope_width + ROT), jnp.float32), -12.0, 12.0)
    return drawn.reshape(TOKENS, head_count * (nope_width + ROT))


def draw_rope_key(key, part):
    return planted_rows(key)[2].astype(jnp.bfloat16)


def draw_query_wide(key, part):
    return planted_query(key, HEADS_W, NOPE_W, 201).astype(jnp.bfloat16)


def draw_query_narrow(key, part):
    return planted_query(key, HEADS_N, NOPE_N, 202).astype(jnp.bfloat16)


def block_scale(key, dims, shards, least, top_value):
    def one(axis_at, blocks):
        steps = jax.random.uniform(jax.random.fold_in(jax.random.fold_in(key, 6), axis_at), (blocks,), jnp.float32, least / len(shards), top_value / len(shards))
        return jnp.repeat(jnp.exp(steps), dims[axis_at] // blocks).reshape((-1,) + (1,) * (len(dims) - axis_at - 1))

    loudness = one(*shards[0])
    for cut in shards[1:]:
        loudness = loudness * one(*cut)
    return loudness


def centred(stream_key, extent, deviation, bound, cuts=(), kind=jnp.bfloat16):
    values = deviation * jax.random.normal(stream_key, extent, jnp.float32)
    if cuts:
        values = values * block_scale(stream_key, extent, cuts, -0.22, 0.18)
    return jnp.clip(values, -bound, bound).astype(kind)


def setup_inputs(seed: int = 0, part: int = 0) -> dict:
    key_of = jax.random.split(jax.random.key(seed), 17)
    own_keys = jax.random.split(jax.random.fold_in(key_of[16], part), 17)
    return {
        "layer_input": centred(own_keys[0], (TOKENS, D), 1.0, 6.0, ((0, 16),)),
        "latent": centred(own_keys[1], (TOKENS, LATENT), 1.0, 6.0, ((0, 8),)),
        "rope_key": draw_rope_key(jax.random.fold_in(jax.random.fold_in(key_of[16], part), 71), part),
        "query_wide": draw_query_wide(jax.random.fold_in(jax.random.fold_in(key_of[16], part), 71), part),
        "query_narrow": draw_query_narrow(jax.random.fold_in(jax.random.fold_in(key_of[16], part), 71), part),
        "key_up_wide": centred(key_of[5], (LATENT, HEADS_W * NOPE_W), LATENT ** -0.5, 0.25, ((1, 2),)),
        "value_up_wide": centred(key_of[6], (LATENT, HEADS_W * VAL_W), LATENT ** -0.5, 0.25, ((1, 2),)),
        "key_up_narrow": centred(key_of[7], (LATENT, HEADS_N * NOPE_N), LATENT ** -0.5, 0.25, ((1, 2),)),
        "value_up_narrow": centred(key_of[8], (LATENT, HEADS_N * VAL_N), LATENT ** -0.5, 0.25, ((1, 2),)),
        "out_wide": centred(key_of[9], (HEADS_W * VAL_W, D), 0.2, 1.1953125, ((0, 2),)),
        "out_narrow": centred(key_of[10], (HEADS_N * VAL_N, D), 0.2, 1.1953125, ((0, 2),)),
        "norm_gain": jnp.clip(1.0 + 0.18 * jax.random.normal(key_of[11], (D,), jnp.float32), 0.1, 1.9),
        "gate_weight": centred(key_of[12], (D, FF), D ** -0.5, 0.125, ((0, 8), (1, 2))),
        "value_weight": centred(key_of[13], (D, FF), D ** -0.5, 0.125, ((0, 8), (1, 2))),
        "conv_weight": centred(key_of[14], (CONV, FF), 0.6, 2.5, ((1, 2),), jnp.float32),
        "down_weight": centred(key_of[15], (FF, D), FF ** -0.5, 0.078125, ((0, 2), (1, 8))),
    }


rope_base = 10000.0
norm_eps = 1e-06

def rope_tables(row_total, span_width):
    places = jnp.arange(row_total, dtype=jnp.int32).astype(jnp.float32)
    frequency = jnp.power(rope_base, -jnp.arange(0, span_width, 2, dtype=jnp.int32).astype(jnp.float32) / span_width)
    angles = places[:, None] * frequency[None, :]
    angles = jnp.concatenate([angles, angles], axis=-1)
    return (jnp.cos(angles), jnp.sin(angles))

def spin_rows(entries, cosine, sine_table):
    entries = entries.astype(jnp.float32)
    lead_half, tail_half = jnp.split(entries, 2, axis=-1)
    return entries * cosine + jnp.concatenate([-tail_half, lead_half], axis=-1) * sine_table

def group_attention(query, latent, turned_key, key_up, value_up, head_count, nope_width, value_width, cosine, sine_table):
    rot_width = turned_key.shape[1]
    shaped = query.reshape(TOKENS, head_count, nope_width + rot_width)
    nope_q = shaped[:, :, :nope_width]
    rope_q = spin_rows(shaped[:, :, nope_width:], cosine[:, None, :], sine_table[:, None, :]).astype(jnp.bfloat16)
    key_rows = jnp.dot(latent, key_up, preferred_element_type=jnp.float32).astype(jnp.bfloat16)
    key_rows = key_rows.reshape(TOKENS, head_count, nope_width).astype(jnp.float32)
    value_rows = jnp.dot(latent, value_up, preferred_element_type=jnp.float32).astype(jnp.bfloat16)
    value_rows = value_rows.reshape(TOKENS, head_count, value_width).astype(jnp.float32)
    key_turned = turned_key.astype(jnp.float32)
    score_scale = 1.0 / math.sqrt(nope_width + rot_width)

    def one_block(query_block):
        nope_block, rope_block = query_block
        scores = jnp.einsum('qhd,khd->qhk', nope_block.astype(jnp.float32), key_rows)
        scores = (scores + jnp.einsum('qhd,kd->qhk', rope_block.astype(jnp.float32), key_turned)) * score_scale
        weights = jnp.exp(scores - lax.optimization_barrier(jnp.max(scores, axis=-1, keepdims=True)))
        row_sum = lax.optimization_barrier(jnp.sum(weights, axis=-1))
        rounded = lax.optimization_barrier(weights.astype(jnp.bfloat16)).astype(jnp.float32)
        mixed = jnp.einsum('qhk,khd->qhd', rounded, value_rows)
        return (mixed / row_sum[:, :, None]).astype(jnp.bfloat16)
    blocks = TOKENS // TOK_DEV
    nope_blocks = nope_q.reshape(blocks, TOK_DEV, head_count, nope_width)
    rope_blocks = rope_q.reshape(blocks, TOK_DEV, head_count, rot_width)
    result = lax.map(one_block, (nope_blocks, rope_blocks))
    return result.reshape(TOKENS, head_count * value_width)

def reference(layer_input, latent, rope_key, query_wide, query_narrow, key_up_wide, value_up_wide, key_up_narrow, value_up_narrow, out_wide, out_narrow, norm_gain, gate_weight, value_weight, conv_weight, down_weight):
    cosine, sine_table = rope_tables(TOKENS, ROT)
    turned_key = spin_rows(rope_key, cosine, sine_table).astype(jnp.bfloat16)
    wide_att = group_attention(query_wide, latent, turned_key, key_up_wide, value_up_wide, HEADS_W, NOPE_W, VAL_W, cosine, sine_table)
    narrow_att = group_attention(query_narrow, latent, turned_key, key_up_narrow, value_up_narrow, HEADS_N, NOPE_N, VAL_N, cosine, sine_table)
    wide_share = HEADS_W * VAL_W // N_TP
    narrow_share = HEADS_N * VAL_N // N_TP
    head_part = jnp.einsum('tic,icd->itd', wide_att.reshape(TOKENS, N_TP, wide_share).astype(jnp.float32), out_wide.reshape(N_TP, wide_share, D).astype(jnp.float32))
    head_part = head_part + jnp.einsum('tic,icd->itd', narrow_att.reshape(TOKENS, N_TP, narrow_share).astype(jnp.float32), out_narrow.reshape(N_TP, narrow_share, D).astype(jnp.float32))
    head_part = lax.optimization_barrier(head_part.astype(jnp.bfloat16)).astype(jnp.float32)
    middle = (layer_input.astype(jnp.float32) + lax.optimization_barrier(jnp.sum(head_part, axis=0))).astype(jnp.bfloat16)
    middle_full = middle.astype(jnp.float32)
    normed = middle_full * lax.rsqrt(lax.optimization_barrier(jnp.mean(middle_full * middle_full, axis=-1, keepdims=True)) + norm_eps)
    normed = (normed * norm_gain).astype(jnp.bfloat16)
    gate_pre = jnp.dot(normed, gate_weight, preferred_element_type=jnp.float32).astype(jnp.bfloat16)
    value_pre = jnp.dot(normed, value_weight, preferred_element_type=jnp.float32)
    padded = jnp.pad(gate_pre, ((1, 1), (0, 0))).astype(jnp.float32)
    conv_gate = jnp.zeros((TOKENS, FF), jnp.float32)
    for kernel_tap in range(CONV):
        conv_gate = conv_gate + conv_weight[kernel_tap] * padded[kernel_tap:kernel_tap + TOKENS]
    hidden = (jax.nn.silu(conv_gate) * value_pre).astype(jnp.bfloat16)
    hidden_share = FF // N_TP
    channel_part = jnp.einsum('tic,icd->itd', hidden.reshape(TOKENS, N_TP, hidden_share).astype(jnp.float32), down_weight.reshape(N_TP, hidden_share, D).astype(jnp.float32))
    channel_part = lax.optimization_barrier(channel_part.astype(jnp.bfloat16)).astype(jnp.float32)
    return (middle_full + lax.optimization_barrier(jnp.sum(channel_part, axis=0))).astype(jnp.bfloat16)
```

```python
import math

import jax
import jax.numpy as jnp
from jax import lax
from jax.sharding import PartitionSpec as P

NOPE_W = 128
NOPE_N = 64


rope_base = 10000.0
norm_eps = 1e-06


def shifted(x, axis, step, size):
    return lax.ppermute(x, axis, [(i, (i + step) % size) for i in range(size)])


def swapped_cores(x):
    size = lax.axis_size("sp")
    return lax.ppermute(x, "sp", [(i, i + 1 - 2 * (i % 2)) for i in range(size)])


def block_at(x, index, width, axis):
    return lax.dynamic_slice_in_dim(x, index * width, width, axis=axis)


def gather_tp(x):
    size, me = lax.axis_size("tp"), lax.axis_index("tp")
    rows = x.shape[0]
    full = jnp.zeros((size * rows, x.shape[1]), x.dtype)
    full = lax.dynamic_update_slice_in_dim(full, x, me * rows, axis=0)
    for step in range(1, size):
        piece = shifted(x, "tp", step, size)
        full = lax.dynamic_update_slice_in_dim(
            full, piece, ((me - step) % size) * rows, axis=0
        )
    return full


def scatter_tp(x):
    size, me = lax.axis_size("tp"), lax.axis_index("tp")
    rows = x.shape[0] // size
    total = block_at(x, me, rows, 0).astype(jnp.float32)
    for step in range(1, size):
        piece = shifted(block_at(x, (me + step) % size, rows, 0), "tp", step, size)
        total = total + piece.astype(jnp.float32)
    return total


def spread_weight(own, theirs, hops):
    planes = lax.axis_size("grp") == 2
    size = lax.axis_size("sp")
    first = lax.axis_index("grp") == 0
    pieces = [(own, theirs)]
    if not planes:
        for _ in range(1, hops):
            own, theirs = (shifted(own, "sp", 2, size), shifted(theirs, "sp", 2, size))
            pieces.append((own, theirs))
        return pieces
    moving = jnp.where(first, own, theirs)
    still = jnp.where(first, theirs, own)
    pieces = [(moving, still)]
    for _ in range(1, hops):
        moving = shifted(moving, "sp", 2, size)
        pieces.append((moving, shifted(moving, "grp", 1, 2)))
    return pieces


def rope_tables(row_start, row_total, span_width):
    places = (row_start + jnp.arange(row_total, dtype=jnp.int32)).astype(jnp.float32)
    frequency = jnp.power(
        rope_base, -jnp.arange(0, span_width, 2, dtype=jnp.int32).astype(jnp.float32) / span_width
    )
    angles = places[:, None] * frequency[None, :]
    angles = jnp.concatenate([angles, angles], axis=-1)
    return (jnp.cos(angles), jnp.sin(angles))


def spin_rows(entries, cosine, sine_table):
    entries = entries.astype(jnp.float32)
    lead_half, tail_half = jnp.split(entries, 2, axis=-1)
    return entries * cosine + jnp.concatenate([-tail_half, lead_half], axis=-1) * sine_table


def prepare_queries(queries, head_count, nope_width, rot_width, cosine, sine_table):
    shaped = queries.reshape(queries.shape[0], head_count, nope_width + rot_width)
    turned = spin_rows(
        shaped[:, :, nope_width:], cosine[:, None, :], sine_table[:, None, :]
    ).astype(jnp.bfloat16)
    return (shaped[:, :, :nope_width], turned)


def start_state(row_total, head_count, value_width):
    return (
        jnp.full((row_total, head_count), -jnp.inf, jnp.float32),
        jnp.zeros((row_total, head_count), jnp.float32),
        jnp.zeros((row_total, head_count, value_width), jnp.float32),
    )


def fold_group(carried, latent_piece, rope_piece, nope_q, rope_q, key_up, value_up, score_scale):
    row_max, row_sum, weighted = carried
    piece_rows = latent_piece.shape[0]
    head_count = nope_q.shape[1]
    key_rows = jnp.dot(latent_piece, key_up, preferred_element_type=jnp.float32).astype(
        jnp.bfloat16
    )
    key_rows = key_rows.reshape(piece_rows, head_count, -1)
    value_rows = jnp.dot(latent_piece, value_up, preferred_element_type=jnp.float32).astype(
        jnp.bfloat16
    )
    value_rows = value_rows.reshape(piece_rows, head_count, -1)
    scores = jnp.einsum("qhd,khd->qhk", nope_q, key_rows, preferred_element_type=jnp.float32)
    scores = (
        scores + jnp.einsum("qhd,kd->qhk", rope_q, rope_piece, preferred_element_type=jnp.float32)
    ) * score_scale
    new_max = jnp.max(scores, axis=-1)
    shrink = jnp.exp(row_max - new_max)
    weights = jnp.exp(scores - new_max[:, :, None])
    row_sum = row_sum * shrink + jnp.sum(weights, axis=-1)
    weighted = weighted * shrink[:, :, None] + jnp.einsum(
        "qhk,khd->qhd", weights.astype(jnp.bfloat16), value_rows, preferred_element_type=jnp.float32
    )
    return (new_max, row_sum, weighted)


def finish_group(carried):
    row_max, row_sum, weighted = carried
    return (weighted / row_sum[:, :, None]).reshape(weighted.shape[0], -1).astype(jnp.bfloat16)


def on_device(
    layer_input,
    latent,
    rope_key,
    query_wide,
    query_narrow,
    key_up_wide,
    value_up_wide,
    key_up_narrow,
    value_up_narrow,
    out_wide,
    out_narrow,
    norm_gain,
    gate_weight,
    value_weight,
    conv_weight,
    down_weight,
):
    seq_rows = latent.shape[0]
    rot_width = rope_key.shape[1]
    hops = lax.axis_size("sp") // 2
    core = lax.axis_index("sp") % 2
    chip = lax.axis_index("sp") // 2
    plane = lax.axis_index("grp") if lax.axis_size("grp") == 2 else 0
    hidden_width = gate_weight.shape[1] // 2
    depth = gate_weight.shape[0]
    out_width = down_weight.shape[1]
    gate_pieces = spread_weight(
        block_at(gate_weight, core, hidden_width, 1),
        swapped_cores(block_at(gate_weight, 1 - core, hidden_width, 1)),
        hops,
    )
    value_pieces = spread_weight(
        block_at(value_weight, core, hidden_width, 1),
        swapped_cores(block_at(value_weight, 1 - core, hidden_width, 1)),
        hops,
    )
    down_pieces = spread_weight(
        block_at(down_weight, core, hidden_width, 0),
        swapped_cores(block_at(down_weight, 1 - core, hidden_width, 0)),
        hops,
    )
    taps = block_at(conv_weight, core, hidden_width, 1)
    row_start = lax.axis_index("sp") * seq_rows
    cosine, sine_table = rope_tables(row_start, seq_rows, rot_width)
    turned_key = spin_rows(rope_key, cosine, sine_table).astype(jnp.bfloat16)
    wide_heads = key_up_wide.shape[1] // NOPE_W
    narrow_heads = key_up_narrow.shape[1] // NOPE_N
    wide_nope, wide_rope = prepare_queries(
        query_wide, wide_heads, NOPE_W, rot_width, cosine, sine_table
    )
    narrow_nope, narrow_rope = prepare_queries(
        query_narrow, narrow_heads, NOPE_N, rot_width, cosine, sine_table
    )
    wide_scale = 1.0 / math.sqrt(NOPE_W + rot_width)
    narrow_scale = 1.0 / math.sqrt(NOPE_N + rot_width)
    initial = (
        start_state(seq_rows, wide_heads, value_up_wide.shape[1] // wide_heads),
        start_state(seq_rows, narrow_heads, value_up_narrow.shape[1] // narrow_heads),
    )
    joined = lax.all_gather(
        jnp.concatenate((latent, turned_key), axis=1), "sp", axis=0, tiled=True
    )
    latent_piece = joined[:, : latent.shape[1]]
    rope_piece = joined[:, latent.shape[1] :]
    wide_state = fold_group(
        initial[0],
        latent_piece,
        rope_piece,
        wide_nope,
        wide_rope,
        key_up_wide,
        value_up_wide,
        wide_scale,
    )
    narrow_state = fold_group(
        initial[1],
        latent_piece,
        rope_piece,
        narrow_nope,
        narrow_rope,
        key_up_narrow,
        value_up_narrow,
        narrow_scale,
    )
    wide_out = finish_group(wide_state)
    narrow_out = finish_group(narrow_state)
    attended = scatter_tp(
        (
            jnp.dot(wide_out, out_wide, preferred_element_type=jnp.float32)
            + jnp.dot(narrow_out, out_narrow, preferred_element_type=jnp.float32)
        ).astype(jnp.bfloat16)
    )
    middle = (layer_input.astype(jnp.float32) + attended).astype(jnp.bfloat16)
    middle_full = middle.astype(jnp.float32)
    normed = middle_full * lax.rsqrt(
        jnp.mean(middle_full * middle_full, axis=-1, keepdims=True) + norm_eps
    )
    normed = (normed * norm_gain).astype(jnp.bfloat16)
    mine = gather_tp(normed)
    other = swapped_cores(mine)
    all_rows = jnp.where(
        core == 0,
        jnp.concatenate((mine, other), axis=0),
        jnp.concatenate((other, mine), axis=0),
    )
    owners = (core + plane) % 2, (core + 1 + plane) % 2
    gate_pre = value_pre = None
    for step in range(hops):
        source = (chip - step) % hops
        for k in range(2):
            columns = block_at(all_rows, 2 * source + owners[k], depth, 1)
            gate_term = jnp.dot(columns, gate_pieces[step][k], preferred_element_type=jnp.float32)
            value_term = jnp.dot(
                columns, value_pieces[step][k], preferred_element_type=jnp.float32
            )
            gate_pre = gate_term if gate_pre is None else gate_pre + gate_term
            value_pre = value_term if value_pre is None else value_pre + value_term
    gate_pre = gate_pre.astype(jnp.bfloat16)
    chip_rows = gate_pre.shape[0]
    up = [(i, i + 2) for i in range(2 * hops - 2)]
    down = [(j, i) for i, j in up]
    before = lax.ppermute(gate_pre[chip_rows - 1 :], "sp", up)
    after = lax.ppermute(gate_pre[:1], "sp", down)
    padded = jnp.concatenate([before, gate_pre, after], axis=0)
    conv_gate = jnp.zeros(gate_pre.shape, jnp.float32)
    for kernel_tap in range(taps.shape[0]):
        conv_gate = conv_gate + taps[kernel_tap] * padded[
            kernel_tap : kernel_tap + chip_rows
        ].astype(jnp.float32)
    hidden = (jax.nn.silu(conv_gate) * value_pre).astype(jnp.bfloat16)
    terms = jnp.zeros((chip_rows, 2 * hops * out_width), jnp.float32)
    for step in range(hops):
        source = (chip - step) % hops
        for k in range(2):
            term = jnp.dot(hidden, down_pieces[step][k], preferred_element_type=jnp.float32)
            terms = lax.dynamic_update_slice_in_dim(
                terms, term, (2 * source + owners[k]) * out_width, axis=1
            )
    theirs = swapped_cores(block_at(terms, 1 - core, seq_rows, 0).astype(jnp.bfloat16))
    part = block_at(terms, core, seq_rows, 0) + theirs.astype(jnp.float32)
    summed = scatter_tp(part.astype(jnp.bfloat16))
    return (middle_full + summed).astype(jnp.bfloat16)


def solution(mesh):
    in_specs = (
        P(("grp", "sp", "tp"), None),
        P(("grp", "sp"), None),
        P(("grp", "sp"), None),
        P(("grp", "sp"), "tp"),
        P(("grp", "sp"), "tp"),
        P(None, "tp"),
        P(None, "tp"),
        P(None, "tp"),
        P(None, "tp"),
        P("tp", None),
        P("tp", None),
        P(),
        P("sp", "tp"),
        P("sp", "tp"),
        P(None, "tp"),
        P("tp", "sp"),
    )
    out_specs = P(("grp", "sp", "tp"), None)
    return jax.shard_map(
        on_device, mesh=mesh, in_specs=in_specs, out_specs=out_specs, check_vma=False
    )
```

```python
import math

import jax
import jax.numpy as jnp
from jax import lax
from jax.sharding import PartitionSpec as P


NOPE_W = 128
NOPE_N = 64


rope_base = 10000.0
norm_eps = 1e-06


def shifted(x, axis, step, size):
    return lax.ppermute(x, axis, [(i, (i + step) % size) for i in range(size)])


def swapped_cores(x):
    size = lax.axis_size("sp")
    return lax.ppermute(x, "sp", [(i, i + 1 - 2 * (i % 2)) for i in range(size)])


def block_at(x, index, width, axis):
    return lax.dynamic_slice_in_dim(x, index * width, width, axis=axis)


def gather_tp(x):
    size, me = lax.axis_size("tp"), lax.axis_index("tp")
    rows = x.shape[0]
    full = jnp.zeros((size * rows, x.shape[1]), x.dtype)
    full = lax.dynamic_update_slice_in_dim(full, x, me * rows, axis=0)
    for step in range(1, size):
        piece = shifted(x, "tp", step, size)
        full = lax.dynamic_update_slice_in_dim(
            full, piece, ((me - step) % size) * rows, axis=0
        )
    return full


def scatter_tp(x):
    size, me = lax.axis_size("tp"), lax.axis_index("tp")
    rows = x.shape[0] // size
    total = block_at(x, me, rows, 0).astype(jnp.float32)
    for step in range(1, size):
        piece = shifted(block_at(x, (me + step) % size, rows, 0), "tp", step, size)
        total = total + piece.astype(jnp.float32)
    return total


def spread_weight(own, theirs, hops):
    planes, size = lax.axis_size("grp"), lax.axis_size("sp")
    pairs = []
    for plane in range(planes):
        for index in range(size):
            across = index + 1 - 2 * (index % 2)
            pairs.append((plane * size + index, (planes - 1 - plane) * size + across))
    pieces = [(own, theirs)]
    for _ in range(1, hops):
        own = shifted(own, "sp", 2, size)
        theirs = lax.ppermute(own, ("grp", "sp"), pairs)
        pieces.append((own, theirs))
    return pieces


def rope_tables(row_start, row_total, span_width):
    places = (row_start + jnp.arange(row_total, dtype=jnp.int32)).astype(jnp.float32)
    frequency = jnp.power(
        rope_base, -jnp.arange(0, span_width, 2, dtype=jnp.int32).astype(jnp.float32) / span_width
    )
    angles = places[:, None] * frequency[None, :]
    angles = jnp.concatenate([angles, angles], axis=-1)
    return (jnp.cos(angles), jnp.sin(angles))


def spin_rows(entries, cosine, sine_table):
    entries = entries.astype(jnp.float32)
    lead_half, tail_half = jnp.split(entries, 2, axis=-1)
    return entries * cosine + jnp.concatenate([-tail_half, lead_half], axis=-1) * sine_table


def prepare_queries(queries, head_count, nope_width, rot_width, cosine, sine_table):
    shaped = queries.reshape(queries.shape[0], head_count, nope_width + rot_width)
    turned = spin_rows(
        shaped[:, :, nope_width:], cosine[:, None, :], sine_table[:, None, :]
    ).astype(jnp.bfloat16)
    return (shaped[:, :, :nope_width], turned)


def start_state(row_total, head_count, value_width):
    return (
        jnp.full((row_total, head_count), -jnp.inf, jnp.float32),
        jnp.zeros((row_total, head_count), jnp.float32),
        jnp.zeros((row_total, head_count, value_width), jnp.float32),
    )


def fold_group(carried, latent_piece, rope_piece, nope_q, rope_q, key_up, value_up, score_scale):
    row_max, row_sum, weighted = carried
    piece_rows = latent_piece.shape[0]
    head_count = nope_q.shape[1]
    key_rows = jnp.dot(latent_piece, key_up, preferred_element_type=jnp.float32).astype(
        jnp.bfloat16
    )
    key_rows = key_rows.reshape(piece_rows, head_count, -1)
    value_rows = jnp.dot(latent_piece, value_up, preferred_element_type=jnp.float32).astype(
        jnp.bfloat16
    )
    value_rows = value_rows.reshape(piece_rows, head_count, -1)
    scores = jnp.einsum("qhd,khd->qhk", nope_q, key_rows, preferred_element_type=jnp.float32)
    scores = (
        scores + jnp.einsum("qhd,kd->qhk", rope_q, rope_piece, preferred_element_type=jnp.float32)
    ) * score_scale
    new_max = jnp.max(scores, axis=-1)
    shrink = jnp.exp(row_max - new_max)
    weights = jnp.exp(scores - new_max[:, :, None])
    row_sum = row_sum * shrink + jnp.sum(weights, axis=-1)
    weighted = weighted * shrink[:, :, None] + jnp.einsum(
        "qhk,khd->qhd", weights.astype(jnp.bfloat16), value_rows, preferred_element_type=jnp.float32
    )
    return (new_max, row_sum, weighted)


def finish_group(carried):
    _, row_sum, weighted = carried
    return (weighted / row_sum[:, :, None]).reshape(weighted.shape[0], -1).astype(jnp.bfloat16)


def layer(
    layer_input,
    latent,
    rope_key,
    query_wide,
    query_narrow,
    key_up_wide,
    value_up_wide,
    key_up_narrow,
    value_up_narrow,
    out_wide,
    out_narrow,
    norm_gain,
    gate_weight,
    value_weight,
    conv_weight,
    down_weight,
):
    seq_rows = latent.shape[0]
    rot_width = rope_key.shape[1]
    hops = lax.axis_size("sp") // 2
    core = lax.axis_index("sp") % 2
    chip = lax.axis_index("sp") // 2
    half = (core + lax.axis_index("grp")) % 2
    hidden_width = gate_weight.shape[1] // 2
    depth = gate_weight.shape[0]
    out_width = down_weight.shape[1]
    gate_pieces = spread_weight(
        block_at(gate_weight, half, hidden_width, 1),
        swapped_cores(block_at(gate_weight, 1 - half, hidden_width, 1)),
        hops,
    )
    value_pieces = spread_weight(
        block_at(value_weight, half, hidden_width, 1),
        swapped_cores(block_at(value_weight, 1 - half, hidden_width, 1)),
        hops,
    )
    down_pieces = spread_weight(
        block_at(down_weight, half, hidden_width, 0),
        swapped_cores(block_at(down_weight, 1 - half, hidden_width, 0)),
        hops,
    )
    taps = block_at(conv_weight, half, hidden_width, 1)
    row_start = lax.axis_index("sp") * seq_rows
    cosine, sine_table = rope_tables(row_start, seq_rows, rot_width)
    turned_key = spin_rows(rope_key, cosine, sine_table).astype(jnp.bfloat16)
    wide_heads = key_up_wide.shape[1] // NOPE_W
    narrow_heads = key_up_narrow.shape[1] // NOPE_N
    wide_nope, wide_rope = prepare_queries(
        query_wide, wide_heads, NOPE_W, rot_width, cosine, sine_table
    )
    narrow_nope, narrow_rope = prepare_queries(
        query_narrow, narrow_heads, NOPE_N, rot_width, cosine, sine_table
    )
    wide_scale = 1.0 / math.sqrt(NOPE_W + rot_width)
    narrow_scale = 1.0 / math.sqrt(NOPE_N + rot_width)
    initial = (
        start_state(seq_rows, wide_heads, value_up_wide.shape[1] // wide_heads),
        start_state(seq_rows, narrow_heads, value_up_narrow.shape[1] // narrow_heads),
    )
    joined = lax.all_gather(
        jnp.concatenate((latent, turned_key), axis=1), "sp", axis=0, tiled=True
    )
    latent_piece = joined[:, : latent.shape[1]]
    rope_piece = joined[:, latent.shape[1] :]
    wide_state = fold_group(
        initial[0],
        latent_piece,
        rope_piece,
        wide_nope,
        wide_rope,
        key_up_wide,
        value_up_wide,
        wide_scale,
    )
    narrow_state = fold_group(
        initial[1],
        latent_piece,
        rope_piece,
        narrow_nope,
        narrow_rope,
        key_up_narrow,
        value_up_narrow,
        narrow_scale,
    )
    wide_out = finish_group(wide_state)
    narrow_out = finish_group(narrow_state)
    attended = scatter_tp(
        (
            jnp.dot(wide_out, out_wide, preferred_element_type=jnp.float32)
            + jnp.dot(narrow_out, out_narrow, preferred_element_type=jnp.float32)
        ).astype(jnp.bfloat16)
    )
    middle = (layer_input.astype(jnp.float32) + attended).astype(jnp.bfloat16)
    middle_full = middle.astype(jnp.float32)
    normed = middle_full * lax.rsqrt(
        jnp.mean(middle_full * middle_full, axis=-1, keepdims=True) + norm_eps
    )
    normed = (normed * norm_gain).astype(jnp.bfloat16)
    mine = gather_tp(normed)
    other = swapped_cores(mine)
    all_rows = jnp.where(
        core == 0,
        jnp.concatenate((mine, other), axis=0),
        jnp.concatenate((other, mine), axis=0),
    )
    owners = core, 1 - core
    gate_pre = value_pre = None
    for step in range(hops):
        source = (chip - step) % hops
        for k in range(2):
            columns = block_at(all_rows, 2 * source + owners[k], depth, 1)
            gate_term = jnp.dot(columns, gate_pieces[step][k], preferred_element_type=jnp.float32)
            value_term = jnp.dot(columns, value_pieces[step][k], preferred_element_type=jnp.float32)
            gate_pre = gate_term if gate_pre is None else gate_pre + gate_term
            value_pre = value_term if value_pre is None else value_pre + value_term
    gate_pre = gate_pre.astype(jnp.bfloat16)
    chip_rows = gate_pre.shape[0]
    up = [(i, i + 2) for i in range(2 * hops - 2)]
    down = [(j, i) for i, j in up]
    before = lax.ppermute(gate_pre[chip_rows - 1 :], "sp", up)
    after = lax.ppermute(gate_pre[:1], "sp", down)
    padded = jnp.concatenate([before, gate_pre, after], axis=0)
    conv_gate = jnp.zeros(gate_pre.shape, jnp.float32)
    for kernel_tap in range(taps.shape[0]):
        conv_gate = conv_gate + taps[kernel_tap] * padded[
            kernel_tap : kernel_tap + chip_rows
        ].astype(jnp.float32)
    hidden = (jax.nn.silu(conv_gate) * value_pre).astype(jnp.bfloat16)
    summed = jnp.zeros(middle_full.shape, jnp.float32)
    for steps in (range(hops - 1), range(hops - 1, hops)):
        if not len(steps):
            continue
        terms = [
            [
                jnp.dot(hidden, down_pieces[step][k], preferred_element_type=jnp.float32)
                for k in range(2)
            ]
            for step in steps
        ]
        leaving = [block_at(pair[1 - k], 1 - core, seq_rows, 0) for pair in terms for k in range(2)]
        staying = [block_at(pair[k], core, seq_rows, 0) for pair in terms for k in range(2)]
        theirs = swapped_cores(jnp.concatenate(leaving, axis=1).astype(jnp.bfloat16))
        part = jnp.concatenate(staying, axis=1) + theirs.astype(jnp.float32)
        part = scatter_tp(part.astype(jnp.bfloat16))
        for place, step in enumerate(steps):
            source = (chip - step) % hops
            for k in range(2):
                summed = lax.dynamic_update_slice_in_dim(
                    summed,
                    lax.slice_in_dim(
                        part, (2 * place + k) * out_width, (2 * place + k + 1) * out_width, axis=1
                    ),
                    (2 * source + owners[k]) * out_width,
                    axis=1,
                )
    return (middle_full + summed).astype(jnp.bfloat16)


def solution(mesh):
    in_specs = (
        P(("grp", "sp", "tp"), None),
        P(("grp", "sp"), None),
        P(("grp", "sp"), None),
        P(("grp", "sp"), "tp"),
        P(("grp", "sp"), "tp"),
        P(None, "tp"),
        P(None, "tp"),
        P(None, "tp"),
        P(None, "tp"),
        P("tp", None),
        P("tp", None),
        P(),
        P("sp", "tp"),
        P("sp", "tp"),
        P(None, "tp"),
        P("tp", "sp"),
    )
    out_specs = P(("grp", "sp", "tp"), None)
    return jax.shard_map(layer, mesh=mesh, in_specs=in_specs, out_specs=out_specs, check_vma=False)
```
